32 devices in a mesh: sp: 8 (over z, x), tp: 4 (over y, core).
Axes of the slice: x: 2, y: 2, z: 4, core: 2. Of those that a mesh axis runs over, the one named last changes fastest.
Arguments:
- residual_signal: bfloat16 [1024, 2048], P('sp', 'tp'), may hold values from -90 to 90
- lifted_signal: bfloat16 [1024, 1024], P('sp', 'tp'), may hold values from -6 to 6
- discrete_timestep: float32 [64, 1024], P('tp', 'sp'), may hold values from 0.17 to 4.2
- additional_log_fading: float32 [64, 1024], P('tp', 'sp'), may hold values from -2.1 to 0
- paired_fading: float32 [2, 32, 64], replicated, may hold values from 1.953125e-05 to 0.0625
- unpaired_fading: float32 [2, 32, 32], replicated, may hold values from 1.953125e-05 to 0.0625
- paired_twist: float32 [2, 32, 64], replicated, may hold values from -3.140625 to 3.140625
- unpaired_twist: float32 [2, 32, 32], replicated, may hold values from -3.140625 to 3.140625
- paired_latent_linears: float32 [2, 2, 2, 32, 64, 16], replicated, may hold values from -1 to 1
- unpaired_latent_linears: float32 [2, 2, 2, 32, 32, 16], replicated, may hold values from -1 to 1
- skip_coefficient: float32 [1024], replicated, may hold values from -4 to 4
- closing_norm_multiplier: float32 [1024], replicated, may hold values from 0.1 to 1.9
- emitted_linear: bfloat16 [1024, 2048], replicated, may hold values from -0.1875 to 0.1875
- leading_norm_multiplier: float32 [2048], replicated, may hold values from 0.1 to 1.9
- raising_linear: bfloat16 [2048, 8192], P('sp', 'tp'), may hold values from -0.125 to 0.125
- lowering_linear: bfloat16 [8192, 2048], P('tp', 'sp'), may hold values from -0.0625 to 0.0625
Outputs:
- layer_out: bfloat16 [1024, 2048], P('sp', 'tp')
The draws below stay inside these ranges and needn't reach their ends.
All inputs are finite; a program needn't handle non-finite values.
Results may differ from the reference program's by a relative error of at most 0.008.
Values may be sent and summed in bfloat16 or wider, within the bound.
A program may use at most 128 MiB of HBM per device.

```python
import math
import jax
import jax.numpy as jnp
from jax import lax

D = 2048
FF = 8192
MIXER_BANDS = 64
CHAN = 16
STATE_LONG = 64
STATE_SHORT = 32
NORM_W = 128
TOK_DEV = 128
SSM_W = 1024
TOKENS = 1024
N_TP = 4


def draw_residual_signal(key, part):
    keys = jax.random.split(jax.random.fold_in(key, 5), 3)
    column = 0.4 * 10.0 ** (jnp.arange(D, dtype=jnp.float32) / D)
    column = column * jax.random.uniform(keys[0], (D,), jnp.float32, 0.7, 1.4)
    base = jnp.clip(jax.random.normal(keys[1], (TOKENS, D), jnp.float32), -4.0, 4.0)
    row_scale = jnp.exp(jax.random.uniform(keys[2], (TOKENS,), jnp.float32, math.log(0.5), math.log(4.0)))
    return (base * row_scale[:, None] * column[None, :]).astype(jnp.bfloat16)


def draw_discrete_timestep(key, part):
    keys = jax.random.split(jax.random.fold_in(key, 7), 2)
    span = TOK_DEV // 2
    count = TOKENS // span
    lowest, highest, rough_low, rough_high = (0.5, 2.0, 0.5, 1.5)
    factor = jnp.exp(jax.random.uniform(keys[0], (count,), jnp.float32, math.log(lowest), math.log(highest)))
    along = jnp.repeat(factor, span)
    rough = jax.random.uniform(keys[1], (MIXER_BANDS, TOKENS), jnp.float32, rough_low, rough_high)
    return along[None, :] * rough


def draw_additional_log_fading(key, part):
    keys = jax.random.split(jax.random.fold_in(key, 9), 2)
    places = jax.random.randint(keys[0], (MIXER_BANDS, 3), 0, TOKENS)
    values = jax.random.uniform(keys[1], (MIXER_BANDS, 3), jnp.float32, math.log(0.5), math.log(0.8))
    hits = (jnp.arange(TOKENS)[None, None, :] == places[:, :, None]).astype(jnp.float32)
    return jnp.sum(hits * values[:, :, None], axis=1)


def draw_rates(key, states):
    keys = jax.random.split(key, 4)
    share = 8
    quick = jax.random.randint(keys[0], (2, MIXER_BANDS // 2), 0, 16) < share
    quick_rate = jnp.exp(jax.random.uniform(keys[1], (2, MIXER_BANDS // 2), jnp.float32, math.log(0.01), math.log(0.025)))
    slow_rate = jnp.exp(jax.random.uniform(keys[2], (2, MIXER_BANDS // 2), jnp.float32, math.log(0.02), math.log(0.12))) / TOKENS
    base = jnp.where(quick, quick_rate, slow_rate)
    spread = jnp.exp(jax.random.uniform(keys[3], (2, MIXER_BANDS // 2, states), jnp.float32, 0.0, math.log(2.5)))
    return base[:, :, None] * spread


def draw_paired_fading(key, part):
    return draw_rates(jax.random.fold_in(key, 11), STATE_LONG)


def draw_unpaired_fading(key, part):
    return draw_rates(jax.random.fold_in(key, 12), STATE_SHORT)


def level_of(key, dims, cuts, least, high):
    def one(axis_at, parts):
        heights = jax.random.uniform(jax.random.fold_in(jax.random.fold_in(key, 6), axis_at), (parts,), jnp.float32, least / len(cuts), high / len(cuts))
        return jnp.repeat(jnp.exp(heights), dims[axis_at] // parts).reshape((-1,) + (1,) * (len(dims) - axis_at - 1))

    level = one(*cuts[0])
    for cut in cuts[1:]:
        level = level * one(*cut)
    return level


def scatter_about(stream_key, shape, deviation, most, cuts=(), kind=jnp.bfloat16):
    drawn = jax.random.normal(stream_key, shape, jnp.float32) * deviation
    if len(cuts) > 0:
        drawn = level_of(stream_key, shape, cuts, -0.22, 0.18) * drawn
    return jnp.clip(drawn, min=-most, max=most).astype(kind)


def setup_inputs(seed: int = 0) -> dict:
    seeds = jax.random.split(jax.random.key(seed), 17)
    residual_signal = draw_residual_signal(jax.random.fold_in(seeds[16], 71), 0)
    lifted_signal = scatter_about(seeds[1], (TOKENS, SSM_W), 1.0, 6.0, ((0, 8), (1, 4)))
    discrete_timestep = draw_discrete_timestep(jax.random.fold_in(seeds[16], 71), 0)
    additional_log_fading = draw_additional_log_fading(jax.random.fold_in(seeds[16], 71), 0)
    paired_fading = draw_paired_fading(jax.random.fold_in(seeds[16], 71), 0)
    unpaired_fading = draw_unpaired_fading(jax.random.fold_in(seeds[16], 71), 0)
    paired_twist = jnp.clip(jax.random.uniform(seeds[6], (2, MIXER_BANDS // 2, STATE_LONG), jnp.float32, -3.140625, 3.140625), -3.140625, 3.140625)
    unpaired_twist = jnp.clip(jax.random.uniform(seeds[7], (2, MIXER_BANDS // 2, STATE_SHORT), jnp.float32, -3.140625, 3.140625), -3.140625, 3.140625)
    paired_latent_linears = scatter_about(seeds[8], (2, 2, 2, MIXER_BANDS // 2, STATE_LONG, CHAN), (2 * CHAN) ** -0.5, 1.0, (), jnp.float32)
    unpaired_latent_linears = scatter_about(seeds[9], (2, 2, 2, MIXER_BANDS // 2, STATE_SHORT, CHAN), (2 * CHAN) ** -0.5, 1.0, (), jnp.float32)
    skip_coefficient = scatter_about(seeds[10], (SSM_W,), 1.0, 4.0, (), jnp.float32)
    closing_norm_multiplier = jnp.clip(1.0 + 0.18 * jax.random.normal(seeds[11], (SSM_W,), jnp.float32), 0.1, 1.9)
    emitted_linear = scatter_about(seeds[12], (SSM_W, D), SSM_W ** -0.5, 0.1875)
    leading_norm_multiplier = jnp.clip(1.0 + 0.18 * jax.random.normal(seeds[13], (D,), jnp.float32), 0.1, 1.9)
    raising_linear = scatter_about(seeds[14], (D, FF), D ** -0.5, 0.125, ((0, 8), (1, 4)))
    lowering_linear = scatter_about(seeds[15], (FF, D), FF ** -0.5, 0.0625, ((0, 4), (1, 8)))
    return {"residual_signal": residual_signal, "lifted_signal": lifted_signal, "discrete_timestep": discrete_timestep, "additional_log_fading": additional_log_fading, "paired_fading": paired_fading, "unpaired_fading": unpaired_fading, "paired_twist": paired_twist, "unpaired_twist": unpaired_twist, "paired_latent_linears": paired_latent_linears, "unpaired_latent_linears": unpaired_latent_linears, "skip_coefficient": skip_coefficient, "closing_norm_multiplier": closing_norm_multiplier, "emitted_linear": emitted_linear, "leading_norm_multiplier": leading_norm_multiplier, "raising_linear": raising_linear, "lowering_linear": lowering_linear}


EPSILON = 1e-06

def combine_maps(early, later):
    first_re, first_im, base_re, base_im = early
    next_re, next_im, add_re, add_im = later
    return (next_re * first_re - next_im * first_im, next_re * first_im + next_im * first_re, next_re * base_re - next_im * base_im + add_re, next_re * base_im + next_im * base_re + add_im)

def step_maps(group_inputs, pace, surge_entries, decay_rate, turn_rate, input_re, input_im):
    scaled = pace[:, :, None]
    magnitude = jnp.exp(-decay_rate[None] * scaled + surge_entries[:, :, None])
    angle = turn_rate[None] * scaled
    weight_in = jnp.sqrt(-jnp.expm1(-2.0 * decay_rate[None] * scaled))
    drive_re = jnp.einsum('ngj,gpj->ngp', group_inputs, input_re, precision=lax.Precision.HIGHEST) * weight_in
    drive_im = jnp.einsum('ngj,gpj->ngp', group_inputs, input_im, precision=lax.Precision.HIGHEST) * weight_in
    return (magnitude * jnp.cos(angle), magnitude * jnp.sin(angle), drive_re, drive_im)

def readout(state_re, state_im, read_re, read_im):
    return jnp.einsum('ngp,gpj->ngj', state_re, read_re, precision=lax.Precision.HIGHEST) - jnp.einsum('ngp,gpj->ngj', state_im, read_im, precision=lax.Precision.HIGHEST)

def kind_output(group_inputs, pace, surge_entries, decay_rate, turn_rate, projection):
    batch_number = group_inputs.shape[0]
    count = batch_number // TOK_DEV
    width = group_inputs.shape[1]
    states = decay_rate.shape[-1]
    input_blocks = group_inputs.reshape(count, TOK_DEV, width, CHAN)
    pace_blocks = pace.reshape(count, TOK_DEV, width)
    jolt_blocks = surge_entries.reshape(count, TOK_DEV, width)
    result = jnp.zeros((count, TOK_DEV, width, CHAN), jnp.float32)
    for direction in range(2):
        backward = direction == 1
        edge = 0 if backward else -1

        def each_block(carry, pieces, direction=direction, backward=backward, edge=edge):
            block_inputs, block_pace, block_jolts = pieces
            maps = step_maps(block_inputs, block_pace, block_jolts, decay_rate[direction], turn_rate[direction], projection[direction, 0, 0], projection[direction, 0, 1])
            prefix_re, prefix_im, state_re, state_im = lax.associative_scan(combine_maps, maps, reverse=backward, axis=0)
            carry_re, carry_im = carry
            state_re = state_re + prefix_re * carry_re[None] - prefix_im * carry_im[None]
            state_im = state_im + prefix_re * carry_im[None] + prefix_im * carry_re[None]
            values = readout(state_re, state_im, projection[direction, 1, 0], projection[direction, 1, 1])
            return ((state_re[edge], state_im[edge]), values)
        start = (jnp.zeros((width, states), jnp.float32), jnp.zeros((width, states), jnp.float32))
        _, values = lax.scan(each_block, start, (input_blocks, pace_blocks, jolt_blocks), reverse=backward)
        result = result + values
    return result.reshape(batch_number, width, CHAN)

def reference(residual_signal, lifted_signal, discrete_timestep, additional_log_fading, paired_fading, unpaired_fading, paired_twist, unpaired_twist, paired_latent_linears, unpaired_latent_linears, skip_coefficient, closing_norm_multiplier, emitted_linear, leading_norm_multiplier, raising_linear, lowering_linear):
    batch_number = residual_signal.shape[0]
    grouped = lifted_signal.astype(jnp.float32).reshape(batch_number, MIXER_BANDS // 2, 2, CHAN)
    pace = discrete_timestep.T.reshape(batch_number, MIXER_BANDS // 2, 2)
    surge_entries = additional_log_fading.T.reshape(batch_number, MIXER_BANDS // 2, 2)
    long_out = kind_output(grouped[:, :, 0], pace[:, :, 0], surge_entries[:, :, 0], paired_fading, paired_twist, paired_latent_linears)
    short_out = kind_output(grouped[:, :, 1], pace[:, :, 1], surge_entries[:, :, 1], unpaired_fading, unpaired_twist, unpaired_latent_linears)
    ssm_out = jnp.stack([long_out, short_out], axis=2).reshape(batch_number, SSM_W)
    activated = jax.nn.gelu(ssm_out + skip_coefficient[None] * grouped.reshape(batch_number, SSM_W))
    heads = activated.reshape(batch_number, SSM_W // NORM_W, NORM_W)
    heads = heads * lax.rsqrt(lax.optimization_barrier(jnp.mean(heads * heads, axis=2, keepdims=True)) + EPSILON)
    combined_result = (heads.reshape(batch_number, SSM_W) * closing_norm_multiplier[None]).astype(jnp.bfloat16)
    inner_activity = residual_signal.astype(jnp.float32) + jnp.dot(combined_result, emitted_linear, preferred_element_type=jnp.float32)
    scale = lax.rsqrt(lax.optimization_barrier(jnp.mean(inner_activity * inner_activity, axis=1, keepdims=True)) + EPSILON)
    normed = (inner_activity * scale * leading_norm_multiplier[None]).astype(jnp.bfloat16)
    block_width = FF // N_TP
    feed = jnp.zeros((batch_number, D), jnp.float32)
    for member in range(N_TP):
        upward = jnp.dot(normed, raising_linear[:, member * block_width:(member + 1) * block_width], preferred_element_type=jnp.float32)
        hidden = jnp.square(jax.nn.relu(upward)).astype(jnp.bfloat16)
        product = jnp.dot(hidden, lowering_linear[member * block_width:(member + 1) * block_width], preferred_element_type=jnp.float32).astype(jnp.bfloat16)
        feed = feed + product.astype(jnp.float32)
    return (inner_activity + feed).astype(jnp.bfloat16)
```

```python
import functools

import jax
import jax.numpy as jnp
from jax import lax
from jax.experimental import pallas as pl
from jax.experimental.pallas import tpu as pltpu
from jax.sharding import PartitionSpec as P

CHAN = 16
NORM_W = 128
EPSILON = 1e-06
SUB = 8
F32, BF16 = jnp.float32, jnp.bfloat16


def sincos(a):
    k = jnp.floor(a * 0.6366197723675814 + 0.5)
    r = a - k * 1.5703125
    r = r - k * 4.8351287841796875e-4
    r = r - k * 3.138556210e-7
    z = r * r
    s = r + r * z * (-1.6666654611e-1 + z * (8.3321608736e-3 + z * -1.9515295891e-4))
    c = 1.0 - 0.5 * z + z * z * (
        4.166664568298827e-2 + z * (-1.388731625493765e-3 + z * 2.443315711809948e-5)
    )
    half = jnp.floor(k * 0.5)
    odd = (k - 2.0 * half) > 0.5
    half_odd = (half - 2.0 * jnp.floor(half * 0.5)) > 0.5
    cos_v = jnp.where(odd, -s, c)
    sin_v = jnp.where(odd, c, s)
    return jnp.where(half_odd, -cos_v, cos_v), jnp.where(half_odd, -sin_v, sin_v)


def one_minus_exp_neg(u):
    t = jnp.full_like(u, 1.0)
    for m in range(10, 1, -1):
        t = 1.0 - u * (1.0 / m) * t
    return u * t


def cmul(ar, ai, br, bi):
    return ar * br - ai * bi, ar * bi + ai * br


def mixer_body(cfg, x_ref, dt_ref, lf_ref, rates_ref, lin_ref, skip_ref, gain_ref,
               resid_ref, lead_ref, emit_hbm, mid_out, normed_out,
               pace, surge, pre, st, blk, ends, ends_all, cin, mg, rows_in, mrg, emit, resid_in,
               copy_sem, s_ends, r_ends, s_rows, r_rows, s_res, r_res):
    nsp, ntp, n, S, W, G, PL, PS, D = cfg
    L = n // SUB
    half = G // 2
    SL = half * PL
    sp = lax.axis_index("sp")
    tp = lax.axis_index("tp")
    q = n // ntp
    Dl = D // ntp
    MESH = pl.DeviceIdType.MESH

    emit_copy = pltpu.make_async_copy(emit_hbm, emit, copy_sem.at[0])
    emit_copy.start()
    barrier = pltpu.get_barrier_semaphore()
    for k in range(1, nsp):
        pl.semaphore_signal(barrier, inc=1, device_id=(lax.rem(sp + k, nsp), tp), device_id_type=MESH)
    for k in range(1, ntp):
        pl.semaphore_signal(barrier, inc=1, device_id=(sp, lax.rem(tp + k, ntp)), device_id_type=MESH)
    pl.semaphore_wait(barrier, nsp + ntp - 2)

    def res_copy(k):
        to = lax.rem(tp + k, ntp)
        return pltpu.make_async_remote_copy(
            src_ref=resid_ref.at[pl.ds(to * q, q), :], dst_ref=resid_in.at[k - 1],
            send_sem=s_res.at[k - 1], recv_sem=r_res.at[k - 1],
            device_id=(sp, to), device_id_type=MESH)

    for k in range(1, ntp):
        res_copy(k).start()

    lane = lax.broadcasted_iota(jnp.int32, (G, S), 1)
    group = jnp.where(lane < SL, 2 * (lane // PL), 2 * ((lane - SL) // PS) + 1)
    spread = (group == lax.broadcasted_iota(jnp.int32, (G, S), 0)).astype(F32)
    pace[...] = jnp.dot(dt_ref[...], spread, precision=lax.Precision.HIGHEST, preferred_element_type=F32)
    surge[...] = jnp.dot(lf_ref[...], spread, precision=lax.Precision.HIGHEST, preferred_element_type=F32)

    row = lax.broadcasted_iota(jnp.int32, (S, W), 0)
    row_group = jnp.where(row < SL, 2 * (row // PL), 2 * ((row - SL) // PS) + 1)
    mask = row_group == lax.broadcasted_iota(jnp.int32, (S, W), 1) // CHAN
    tile = (lax.broadcasted_iota(jnp.int32, (CHAN, W), 1) % CHAN
            == lax.broadcasted_iota(jnp.int32, (CHAN, W), 0)).astype(BF16)

    def block_map(index, sign=1.0):
        wide = jnp.dot(lin_ref[index].astype(BF16), tile, preferred_element_type=F32)
        return jnp.where(mask, sign * wide, 0.0).astype(BF16)

    xv = x_ref[...]
    for e in range(2):
        for c in range(2):
            st[:, pl.ds((2 * e + c) * S, S)] = lax.dot_general(
                xv, block_map(4 * e + c), (((1,), (1,)), ((), ())), preferred_element_type=F32)

    for e in range(2):
        rate = rates_ref[2 * e : 2 * e + 1, :]
        freq = rates_ref[2 * e + 1 : 2 * e + 2, :]

        def step(i, carry):
            pr, pi, sr, si = carry
            at = i if e == 0 else L - 1 - i
            rows = pl.ds(pl.multiple_of(at * SUB, SUB), SUB)
            d = pace[rows, :]
            rd = rate * d
            m = jnp.exp(surge[rows, :] - rd)
            cos_v, sin_v = sincos(freq * d)
            w = jnp.sqrt(one_minus_exp_neg(2.0 * rd))
            ar, ai = m * cos_v, m * sin_v
            pr, pi = cmul(ar, ai, pr, pi)
            sr, si = cmul(ar, ai, sr, si)
            sr = sr + w * st[rows, pl.ds(2 * e * S, S)]
            si = si + w * st[rows, pl.ds((2 * e + 1) * S, S)]
            pre[rows, pl.ds(2 * e * S, S)] = pr
            pre[rows, pl.ds((2 * e + 1) * S, S)] = pi
            st[rows, pl.ds(2 * e * S, S)] = sr
            st[rows, pl.ds((2 * e + 1) * S, S)] = si
            return pr, pi, sr, si

        zero = jnp.zeros((SUB, S), F32)
        total = lax.fori_loop(0, L, step, (zero + 1.0, zero, zero, zero))
        for c in range(4):
            blk[4 * e + c] = total[c]
        order = range(SUB) if e == 0 else range(SUB - 1, -1, -1)
        run = None
        for b in order:
            now = tuple(blk[4 * e + c, b : b + 1, :] for c in range(4))
            if run is None:
                run = now
            else:
                p = cmul(now[0], now[1], run[0], run[1])
                s = cmul(now[0], now[1], run[2], run[3])
                run = (p[0], p[1], s[0] + now[2], s[1] + now[3])
        for c in range(4):
            ends[4 * e + c : 4 * e + c + 1, :] = run[c]

    def ends_copy(k):
        return pltpu.make_async_remote_copy(
            src_ref=ends, dst_ref=ends_all.at[k - 1],
            send_sem=s_ends.at[k - 1], recv_sem=r_ends.at[k - 1],
            device_id=(lax.rem(sp + k, nsp), tp), device_id_type=MESH)

    for k in range(1, nsp):
        ends_copy(k).start()

    read = jnp.concatenate(
        [block_map(2), block_map(3, -1.0), block_map(6), block_map(7, -1.0)], axis=0)

    for k in range(1, nsp):
        ends_copy(k).wait_recv()
    blank = jnp.zeros((1, S), F32)

    def fold(j, carry, e):
        cr, ci = carry
        k = nsp - 1 - j if e == 0 else j + 1
        reached = k <= sp if e == 0 else nsp - k <= nsp - 1 - sp
        got = ends_all[k - 1]
        nr, ni = cmul(got[4 * e : 4 * e + 1], got[4 * e + 1 : 4 * e + 2], cr, ci)
        nr = nr + got[4 * e + 2 : 4 * e + 3]
        ni = ni + got[4 * e + 3 : 4 * e + 4]
        return jnp.where(reached, nr, cr), jnp.where(reached, ni, ci)

    for e in range(2):
        cr, ci = lax.fori_loop(0, nsp - 1, functools.partial(fold, e=e), (blank, blank))
        order = range(SUB) if e == 0 else range(SUB - 1, -1, -1)
        for b in order:
            cin[2 * e, b : b + 1, :] = cr
            cin[2 * e + 1, b : b + 1, :] = ci
            now = tuple(blk[4 * e + c, b : b + 1, :] for c in range(4))
            nr, ni = cmul(now[0], now[1], cr, ci)
            cr, ci = nr + now[2], ni + now[3]

        inr, ini = cin[2 * e], cin[2 * e + 1]

        def settle(i, _):
            rows = pl.ds(pl.multiple_of(i * SUB, SUB), SUB)
            re, im = pl.ds(2 * e * S, S), pl.ds((2 * e + 1) * S, S)
            ar, ai = cmul(pre[rows, re], pre[rows, im], inr, ini)
            st[rows, re] = st[rows, re] + ar
            st[rows, im] = st[rows, im] + ai
            return 0

        lax.fori_loop(0, L, settle, 0)

    y = jnp.dot(st[...].astype(BF16), read, preferred_element_type=F32)
    y = y + skip_ref[...] * xv.astype(F32)
    y = 0.5 * y * (1.0 + jnp.tanh(0.7978845608028654 * (y + 0.044715 * y * y * y)))
    heads = []
    for h in range(W // NORM_W):
        part = y[:, h * NORM_W : (h + 1) * NORM_W]
        scale = lax.rsqrt(jnp.mean(part * part, axis=1, keepdims=True) + EPSILON)
        heads.append(part * scale * gain_ref[:, h * NORM_W : (h + 1) * NORM_W])
    merged = jnp.concatenate(heads, axis=1).astype(BF16)
    t = lax.broadcasted_iota(jnp.int32, (n, n), 0)
    r = lax.broadcasted_iota(jnp.int32, (n, n), 1)
    unmix = (r == (t % L) * SUB + t // L).astype(BF16)
    mg[...] = jnp.dot(unmix, merged, preferred_element_type=F32).astype(BF16).reshape(ntp, q, W)

    def row_copy(k):
        to = lax.rem(tp + k, ntp)
        return pltpu.make_async_remote_copy(
            src_ref=mg.at[to], dst_ref=rows_in.at[k - 1],
            send_sem=s_rows.at[k - 1], recv_sem=r_rows.at[k - 1],
            device_id=(sp, to), device_id_type=MESH)

    for k in range(1, ntp):
        row_copy(k).start()
    emit_copy.wait()
    mrg[:, pl.ds(pl.multiple_of(tp * W, 128), W)] = mg[tp]
    mid_out[:, pl.ds(pl.multiple_of(tp * Dl, 128), Dl)] = resid_ref[pl.ds(pl.multiple_of(tp * q, q), q), :].astype(F32)
    for k in range(1, ntp):
        src = lax.rem(tp - k + ntp, ntp)
        res_copy(k).wait_recv()
        mid_out[:, pl.ds(pl.multiple_of(src * Dl, 128), Dl)] = resid_in[k - 1].astype(F32)
        row_copy(k).wait_recv()
        mrg[:, pl.ds(pl.multiple_of(src * W, 128), W)] = rows_in[k - 1]
    mid = mid_out[...] + jnp.dot(mrg[...], emit[...], preferred_element_type=F32)
    mid_out[...] = mid
    scale = lax.rsqrt(jnp.mean(mid * mid, axis=1, keepdims=True) + EPSILON)
    normed_out[...] = (mid * scale * lead_ref[...]).astype(BF16)
    for k in range(1, nsp):
        ends_copy(k).wait_send()
    for k in range(1, ntp):
        res_copy(k).wait_send()
        row_copy(k).wait_send()


def on_device(residual, lifted, dts, fades, long_rate, short_rate, long_freq, short_freq,
              long_lin, short_lin, skip, closing, emitted, leading, raising, lowering):
    nsp, ntp = lax.axis_size("sp"), lax.axis_size("tp")
    rank = lax.axis_index("tp")
    n, W = lifted.shape
    G = dts.shape[0]
    half = G // 2
    PL, PS = long_rate.shape[2], short_rate.shape[2]
    S = half * (PL + PS)
    D = emitted.shape[1]
    Dl = residual.shape[1]
    L, q = n // SUB, n // ntp

    def owned(array, axis, count):
        return lax.dynamic_slice_in_dim(array, rank * count, count, axis)

    x = lifted.reshape(SUB, L, W).transpose(1, 0, 2).reshape(n, W)
    mix = lambda a: a.reshape(G, SUB, L).transpose(2, 1, 0).reshape(n, G)
    flat = lambda a, b: jnp.concatenate(
        [owned(a, 1, half).reshape(2, -1), owned(b, 1, half).reshape(2, -1)], axis=1)
    rates = jnp.stack([flat(long_rate, short_rate), flat(long_freq, short_freq)], axis=1).reshape(4, S)
    lin = jnp.concatenate(
        [owned(long_lin, 3, half).reshape(8, half * PL, CHAN),
         owned(short_lin, 3, half).reshape(8, half * PS, CHAN)], axis=1)
    cfg = (nsp, ntp, n, S, W, G, PL, PS, D)
    vm = pl.BlockSpec(memory_space=pltpu.VMEM)
    dma = pltpu.SemaphoreType.DMA
    mid, normed = pl.pallas_call(
        functools.partial(mixer_body, cfg),
        out_shape=(jax.ShapeDtypeStruct((q, D), F32), jax.ShapeDtypeStruct((q, D), BF16)),
        in_specs=[vm] * 9 + [pl.BlockSpec(memory_space=pl.ANY)],
        out_specs=(vm, vm),
        scratch_shapes=[
            pltpu.VMEM((n, S), F32), pltpu.VMEM((n, S), F32),
            pltpu.VMEM((n, 4 * S), F32), pltpu.VMEM((n, 4 * S), F32),
            pltpu.VMEM((8, SUB, S), F32), pltpu.VMEM((8, S), F32), pltpu.VMEM((nsp - 1, 8, S), F32),
            pltpu.VMEM((4, SUB, S), F32),
            pltpu.VMEM((ntp, q, W), BF16), pltpu.VMEM((ntp - 1, q, W), BF16),
            pltpu.VMEM((q, ntp * W), BF16), pltpu.VMEM(emitted.shape, BF16),
            pltpu.VMEM((ntp - 1, q, Dl), BF16),
            dma((1,)), dma((nsp - 1,)), dma((nsp - 1,)), dma((ntp - 1,)), dma((ntp - 1,)),
            dma((ntp - 1,)), dma((ntp - 1,)),
        ],
        compiler_params=pltpu.CompilerParams(collective_id=0, has_side_effects=True),
        cost_estimate=pl.CostEstimate(flops=10**9, bytes_accessed=3 * 10**7, transcendentals=10**6),
    )(x, mix(dts), mix(fades), rates, lin, owned(skip, 0, W)[None], owned(closing, 0, W)[None],
      residual, leading[None], emitted)
    whole_rows = lax.all_gather(normed, "tp", axis=0, tiled=True)
    upward = jnp.dot(whole_rows, lax.all_gather(raising, "sp", axis=0, tiled=True),
                     preferred_element_type=F32)
    hidden = jnp.square(jax.nn.relu(upward)).astype(BF16)
    partial_value = jnp.dot(hidden, lax.all_gather(lowering, "sp", axis=1, tiled=True),
                            preferred_element_type=F32)
    feed = lax.psum_scatter(partial_value.astype(BF16), "tp", scatter_dimension=0, tiled=True).astype(F32)
    out = (mid + feed).astype(BF16)
    return lax.all_to_all(out, "tp", split_axis=1, concat_axis=0, tiled=True)


def solution(mesh):
    both, swapped = P("sp", "tp"), P("tp", "sp")
    in_specs = (both, both, swapped, swapped) + (P(),) * 10 + (both, swapped)
    return jax.shard_map(on_device, mesh=mesh, in_specs=in_specs, out_specs=both, check_vma=False)
```

```python
import functools

import jax
import jax.numpy as jnp
from jax import lax
from jax.experimental import pallas as pl
from jax.experimental.pallas import tpu as pltpu
from jax.sharding import PartitionSpec as P

CHAN = 16
NORM_W = 128
EPSILON = 1e-06
SUB = 8
F32, BF16 = jnp.float32, jnp.bfloat16


def sincos(a):
    k = jnp.floor(a * 0.6366197723675814 + 0.5)
    r = a - k * 1.5703125
    r = r - k * 4.8351287841796875e-4
    r = r - k * 3.138556210e-7
    z = r * r
    s = r + r * z * (-1.6666654611e-1 + z * (8.3321608736e-3 + z * -1.9515295891e-4))
    c = 1.0 - 0.5 * z + z * z * (
        4.166664568298827e-2 + z * (-1.388731625493765e-3 + z * 2.443315711809948e-5)
    )
    half = jnp.floor(k * 0.5)
    odd = (k - 2.0 * half) > 0.5
    half_odd = (half - 2.0 * jnp.floor(half * 0.5)) > 0.5
    cos_v = jnp.where(odd, -s, c)
    sin_v = jnp.where(odd, c, s)
    return jnp.where(half_odd, -cos_v, cos_v), jnp.where(half_odd, -sin_v, sin_v)


def one_minus_exp_neg(u):
    t = jnp.full_like(u, 1.0)
    for m in range(10, 1, -1):
        t = 1.0 - u * (1.0 / m) * t
    return u * t


def cmul(ar, ai, br, bi):
    return ar * br - ai * bi, ar * bi + ai * br


def mixer_body(cfg, x_ref, dt_ref, lf_ref, rates_ref, lin_ref, skip_ref, gain_ref,
               resid_ref, lead_ref, emit_hbm, up_hbm, down_hbm, out_ref,
               pace, surge, pre, st, blk, ends, ends_all, cin, mg, rows_in, mrg, emit, resid_in,
               mid_out, wup, wdn, nrm, hid, part, rs_in, fin, fin_in,
               copy_sem, s_ends, r_ends, s_rows, r_rows, s_res, r_res,
               s_u1, r_u1, s_d1, r_d1, s_u2, r_u2, s_d2, r_d2, s_u3, r_u3, s_d3, r_d3,
               s_nrm, r_nrm, s_rs, r_rs, s_fin, r_fin):
    nsp, ntp, n, S, W, G, PL, PS, D, c_ff, F = cfg
    M = ntp // 2
    L = n // SUB
    half = G // 2
    SL = half * PL
    sp = lax.axis_index("sp")
    tp = lax.axis_index("tp")
    q = n // ntp
    Dl = D // ntp
    MESH = pl.DeviceIdType.MESH

    emit_copy = pltpu.make_async_copy(emit_hbm, emit, copy_sem.at[0])
    emit_copy.start()
    chunk = lax.rem(sp, c_ff)
    partner = tp + 1 - 2 * lax.rem(tp, 2)

    def cols(of):
        return pl.ds(pl.multiple_of(of * F, 128), F)

    own_up = pltpu.make_async_copy(up_hbm.at[:, cols(chunk)], wup.at[tp, sp], copy_sem.at[1])
    own_down = pltpu.make_async_copy(down_hbm.at[cols(chunk), :], wdn.at[tp, sp], copy_sem.at[2])
    own_up.start()
    own_down.start()

    def spread_copy(k, up):
        to = lax.rem(sp + k, nsp)
        src = up_hbm.at[:, cols(lax.rem(to, c_ff))] if up else down_hbm.at[cols(lax.rem(to, c_ff)), :]
        return pltpu.make_async_remote_copy(
            src_ref=src, dst_ref=(wup if up else wdn).at[tp, sp],
            send_sem=(s_u1 if up else s_d1).at[k - 1], recv_sem=(r_u1 if up else r_d1).at[k - 1],
            device_id=(to, tp), device_id_type=MESH)

    def across_copy(m, k, up):
        piece = (wup if up else wdn).at[tp, lax.rem(sp - k + nsp, nsp)]
        return pltpu.make_async_remote_copy(
            src_ref=piece, dst_ref=piece,
            send_sem=(s_u2 if up else s_d2).at[m - 1, k], recv_sem=(r_u2 if up else r_d2).at[m - 1, k],
            device_id=(sp, lax.rem(tp + 2 * m, ntp)), device_id_type=MESH)

    def pair_copy(m, up):
        piece = (wup if up else wdn).at[lax.rem(tp + 2 * m, ntp)]
        return pltpu.make_async_remote_copy(
            src_ref=piece, dst_ref=piece,
            send_sem=(s_u3 if up else s_d3).at[m], recv_sem=(r_u3 if up else r_d3).at[m],
            device_id=(sp, partner), device_id_type=MESH)

    def pass_on(first, last, up):
        for k in range(first, last):
            if k == 0:
                (own_up if up else own_down).wait()
            else:
                spread_copy(k, up).wait_recv()
            for m in range(1, M):
                across_copy(m, k, up).start()

    barrier = pltpu.get_barrier_semaphore()
    for k in range(1, nsp):
        pl.semaphore_signal(barrier, inc=1, device_id=(lax.rem(sp + k, nsp), tp), device_id_type=MESH)
    for k in range(1, ntp):
        pl.semaphore_signal(barrier, inc=1, device_id=(sp, lax.rem(tp + k, ntp)), device_id_type=MESH)
    pl.semaphore_wait(barrier, nsp + ntp - 2)

    def res_copy(k):
        to = lax.rem(tp + k, ntp)
        return pltpu.make_async_remote_copy(
            src_ref=resid_ref.at[pl.ds(to * q, q), :], dst_ref=resid_in.at[k - 1],
            send_sem=s_res.at[k - 1], recv_sem=r_res.at[k - 1],
            device_id=(sp, to), device_id_type=MESH)

    for k in range(1, nsp):
        spread_copy(k, True).start()
    for k in range(1, ntp):
        res_copy(k).start()

    lane = lax.broadcasted_iota(jnp.int32, (G, S), 1)
    group = jnp.where(lane < SL, 2 * (lane // PL), 2 * ((lane - SL) // PS) + 1)
    spread = (group == lax.broadcasted_iota(jnp.int32, (G, S), 0)).astype(F32)
    pace[...] = jnp.dot(dt_ref[...], spread, precision=lax.Precision.HIGHEST, preferred_element_type=F32)
    surge[...] = jnp.dot(lf_ref[...], spread, precision=lax.Precision.HIGHEST, preferred_element_type=F32)

    row = lax.broadcasted_iota(jnp.int32, (S, W), 0)
    row_group = jnp.where(row < SL, 2 * (row // PL), 2 * ((row - SL) // PS) + 1)
    mask = row_group == lax.broadcasted_iota(jnp.int32, (S, W), 1) // CHAN
    tile = (lax.broadcasted_iota(jnp.int32, (CHAN, W), 1) % CHAN
            == lax.broadcasted_iota(jnp.int32, (CHAN, W), 0)).astype(BF16)

    def block_map(index, sign=1.0):
        wide = jnp.dot(lin_ref[index].astype(BF16), tile, preferred_element_type=F32)
        return jnp.where(mask, sign * wide, 0.0).astype(BF16)

    xv = x_ref[...]
    for e in range(2):
        for c in range(2):
            st[:, pl.ds((2 * e + c) * S, S)] = lax.dot_general(
                xv, block_map(4 * e + c), (((1,), (1,)), ((), ())), preferred_element_type=F32)

    for e in range(2):
        rate = rates_ref[2 * e : 2 * e + 1, :]
        freq = rates_ref[2 * e + 1 : 2 * e + 2, :]

        def step(i, carry):
            pr, pi, sr, si = carry
            at = i if e == 0 else L - 1 - i
            rows = pl.ds(pl.multiple_of(at * SUB, SUB), SUB)
            d = pace[rows, :]
            rd = rate * d
            m = jnp.exp(surge[rows, :] - rd)
            cos_v, sin_v = sincos(freq * d)
            w = jnp.sqrt(one_minus_exp_neg(2.0 * rd))
            ar, ai = m * cos_v, m * sin_v
            pr, pi = cmul(ar, ai, pr, pi)
            sr, si = cmul(ar, ai, sr, si)
            sr = sr + w * st[rows, pl.ds(2 * e * S, S)]
            si = si + w * st[rows, pl.ds((2 * e + 1) * S, S)]
            pre[rows, pl.ds(2 * e * S, S)] = pr
            pre[rows, pl.ds((2 * e + 1) * S, S)] = pi
            st[rows, pl.ds(2 * e * S, S)] = sr
            st[rows, pl.ds((2 * e + 1) * S, S)] = si
            return pr, pi, sr, si

        zero = jnp.zeros((SUB, S), F32)
        total = lax.fori_loop(0, L, step, (zero + 1.0, zero, zero, zero))
        for c in range(4):
            blk[4 * e + c] = total[c]
        order = range(SUB) if e == 0 else range(SUB - 1, -1, -1)
        run = None
        for b in order:
            now = tuple(blk[4 * e + c, b : b + 1, :] for c in range(4))
            if run is None:
                run = now
            else:
                p = cmul(now[0], now[1], run[0], run[1])
                s = cmul(now[0], now[1], run[2], run[3])
                run = (p[0], p[1], s[0] + now[2], s[1] + now[3])
        for c in range(4):
            ends[4 * e + c : 4 * e + c + 1, :] = run[c]

    def ends_copy(k):
        return pltpu.make_async_remote_copy(
            src_ref=ends, dst_ref=ends_all.at[k - 1],
            send_sem=s_ends.at[k - 1], recv_sem=r_ends.at[k - 1],
            device_id=(lax.rem(sp + k, nsp), tp), device_id_type=MESH)

    for k in range(1, nsp):
        ends_copy(k).start()
    for k in range(1, nsp):
        spread_copy(k, False).start()

    read = jnp.concatenate(
        [block_map(2), block_map(3, -1.0), block_map(6), block_map(7, -1.0)], axis=0)

    pass_on(0, nsp // 2, True)
    for k in range(1, nsp):
        ends_copy(k).wait_recv()
    blank = jnp.zeros((1, S), F32)

    def fold(j, carry, e):
        cr, ci = carry
        k = nsp - 1 - j if e == 0 else j + 1
        reached = k <= sp if e == 0 else nsp - k <= nsp - 1 - sp
        got = ends_all[k - 1]
        nr, ni = cmul(got[4 * e : 4 * e + 1], got[4 * e + 1 : 4 * e + 2], cr, ci)
        nr = nr + got[4 * e + 2 : 4 * e + 3]
        ni = ni + got[4 * e + 3 : 4 * e + 4]
        return jnp.where(reached, nr, cr), jnp.where(reached, ni, ci)

    for e in range(2):
        cr, ci = lax.fori_loop(0, nsp - 1, functools.partial(fold, e=e), (blank, blank))
        order = range(SUB) if e == 0 else range(SUB - 1, -1, -1)
        for b in order:
            cin[2 * e, b : b + 1, :] = cr
            cin[2 * e + 1, b : b + 1, :] = ci
            now = tuple(blk[4 * e + c, b : b + 1, :] for c in range(4))
            nr, ni = cmul(now[0], now[1], cr, ci)
            cr, ci = nr + now[2], ni + now[3]

        inr, ini = cin[2 * e], cin[2 * e + 1]

        def settle(i, _):
            rows = pl.ds(pl.multiple_of(i * SUB, SUB), SUB)
            re, im = pl.ds(2 * e * S, S), pl.ds((2 * e + 1) * S, S)
            ar, ai = cmul(pre[rows, re], pre[rows, im], inr, ini)
            st[rows, re] = st[rows, re] + ar
            st[rows, im] = st[rows, im] + ai
            return 0

        lax.fori_loop(0, L, settle, 0)

    y = jnp.dot(st[...].astype(BF16), read, preferred_element_type=F32)
    y = y + skip_ref[...] * xv.astype(F32)
    y = 0.5 * y * (1.0 + jnp.tanh(0.7978845608028654 * (y + 0.044715 * y * y * y)))
    heads = []
    for h in range(W // NORM_W):
        head = y[:, h * NORM_W : (h + 1) * NORM_W]
        scale = lax.rsqrt(jnp.mean(head * head, axis=1, keepdims=True) + EPSILON)
        heads.append(head * scale * gain_ref[:, h * NORM_W : (h + 1) * NORM_W])
    merged = jnp.concatenate(heads, axis=1).astype(BF16)
    t = lax.broadcasted_iota(jnp.int32, (n, n), 0)
    r = lax.broadcasted_iota(jnp.int32, (n, n), 1)
    unmix = (r == (t % L) * SUB + t // L).astype(BF16)
    mg[...] = jnp.dot(unmix, merged, preferred_element_type=F32).astype(BF16).reshape(ntp, q, W)

    def row_copy(k):
        to = lax.rem(tp + k, ntp)
        return pltpu.make_async_remote_copy(
            src_ref=mg.at[to], dst_ref=rows_in.at[k - 1],
            send_sem=s_rows.at[k - 1], recv_sem=r_rows.at[k - 1],
            device_id=(sp, to), device_id_type=MESH)

    for k in range(1, ntp):
        row_copy(k).start()
    pass_on(nsp // 2, nsp, True)
    emit_copy.wait()
    mrg[:, pl.ds(pl.multiple_of(tp * W, 128), W)] = mg[tp]
    mid_out[:, pl.ds(pl.multiple_of(tp * Dl, 128), Dl)] = resid_ref[pl.ds(pl.multiple_of(tp * q, q), q), :].astype(F32)
    for k in range(1, ntp):
        src = lax.rem(tp - k + ntp, ntp)
        res_copy(k).wait_recv()
        mid_out[:, pl.ds(pl.multiple_of(src * Dl, 128), Dl)] = resid_in[k - 1].astype(F32)
        row_copy(k).wait_recv()
        mrg[:, pl.ds(pl.multiple_of(src * W, 128), W)] = rows_in[k - 1]
    mid = mid_out[...] + jnp.dot(mrg[...], emit[...], preferred_element_type=F32)
    mid_out[...] = mid
    scale = lax.rsqrt(jnp.mean(mid * mid, axis=1, keepdims=True) + EPSILON)
    base, q_all = sp - chunk, c_ff * q
    nrm[chunk] = (mid * scale * lead_ref[...]).astype(BF16)

    def peer(k):
        return lax.rem(chunk + k, c_ff)

    def nrm_copy(k):
        return pltpu.make_async_remote_copy(
            src_ref=nrm.at[chunk], dst_ref=nrm.at[chunk],
            send_sem=s_nrm.at[k - 1], recv_sem=r_nrm.at[k - 1],
            device_id=(base + peer(k), tp), device_id_type=MESH)

    def rs_copy(k):
        return pltpu.make_async_remote_copy(
            src_ref=part.at[peer(k)], dst_ref=rs_in.at[k - 1],
            send_sem=s_rs.at[k - 1], recv_sem=r_rs.at[k - 1],
            device_id=(base + peer(k), tp), device_id_type=MESH)

    def fin_copy(k):
        to = lax.rem(tp + k, ntp)
        return pltpu.make_async_remote_copy(
            src_ref=fin.at[to], dst_ref=fin_in.at[k - 1],
            send_sem=s_fin.at[k - 1], recv_sem=r_fin.at[k - 1],
            device_id=(sp, to), device_id_type=MESH)

    for k in range(1, c_ff):
        nrm_copy(k).start()
    pair_copy(0, True).start()
    pass_on(0, nsp, False)
    pair_copy(0, False).start()
    for up in (True, False):
        for m in range(1, M):
            for k in range(nsp):
                across_copy(m, k, up).wait_recv()
            pair_copy(M - m, up).start()
        if up:
            for m in range(M):
                pair_copy(m, True).wait_recv()
            for k in range(1, c_ff):
                nrm_copy(k).wait_recv()
            rows = nrm[...].reshape(q_all, D)

            def raise_step(t, _):
                upward = jnp.dot(rows, wup[t].reshape(D, F), preferred_element_type=F32)
                hid[t] = jnp.square(jnp.maximum(upward, 0.0)).astype(BF16)
                return 0

            lax.fori_loop(0, ntp, raise_step, 0)
    for m in range(M):
        pair_copy(m, False).wait_recv()
    Dc = D // nsp
    for j in range(nsp):
        total = jnp.dot(hid[0], wdn[0, j], preferred_element_type=F32)
        for t in range(1, ntp):
            total = total + jnp.dot(hid[t], wdn[t, j], preferred_element_type=F32)
        part[:, :, j * Dc : (j + 1) * Dc] = total.astype(BF16).reshape(c_ff, q, Dc)
    for k in range(1, c_ff):
        rs_copy(k).start()
    result = mid_out[...] + part[chunk].astype(F32)
    for k in range(1, c_ff):
        rs_copy(k).wait_recv()
        result = result + rs_in[k - 1].astype(F32)
    result = result.astype(BF16)
    for t in range(ntp):
        fin[t] = result[:, t * Dl : (t + 1) * Dl]
    for k in range(1, ntp):
        fin_copy(k).start()
    out_ref[pl.ds(pl.multiple_of(tp * q, q), q), :] = fin[tp]
    for k in range(1, ntp):
        fin_copy(k).wait_recv()
        src = lax.rem(tp - k + ntp, ntp)
        out_ref[pl.ds(pl.multiple_of(src * q, q), q), :] = fin_in[k - 1]
    for k in range(1, c_ff):
        nrm_copy(k).wait_send()
        rs_copy(k).wait_send()
    for k in range(1, ntp):
        fin_copy(k).wait_send()
    for up in (True, False):
        for k in range(1, nsp):
            spread_copy(k, up).wait_send()
        for m in range(1, M):
            for k in range(nsp):
                across_copy(m, k, up).wait_send()
        for m in range(M):
            pair_copy(m, up).wait_send()
    for k in range(1, nsp):
        ends_copy(k).wait_send()
    for k in range(1, ntp):
        res_copy(k).wait_send()
        row_copy(k).wait_send()


def on_device(residual, lifted, dts, fades, long_rate, short_rate, long_freq, short_freq,
              long_lin, short_lin, skip, closing, emitted, leading, raising, lowering):
    nsp, ntp = lax.axis_size("sp"), lax.axis_size("tp")
    rank = lax.axis_index("tp")
    n, W = lifted.shape
    G = dts.shape[0]
    half = G // 2
    PL, PS = long_rate.shape[2], short_rate.shape[2]
    S = half * (PL + PS)
    D = emitted.shape[1]
    Dl = residual.shape[1]
    L, q = n // SUB, n // ntp

    def owned(array, axis, count):
        return lax.dynamic_slice_in_dim(array, rank * count, count, axis)

    x = lifted.reshape(SUB, L, W).transpose(1, 0, 2).reshape(n, W)
    mix = lambda a: a.reshape(G, SUB, L).transpose(2, 1, 0).reshape(n, G)
    flat = lambda a, b: jnp.concatenate(
        [owned(a, 1, half).reshape(2, -1), owned(b, 1, half).reshape(2, -1)], axis=1)
    rates = jnp.stack([flat(long_rate, short_rate), flat(long_freq, short_freq)], axis=1).reshape(4, S)
    lin = jnp.concatenate(
        [owned(long_lin, 3, half).reshape(8, half * PL, CHAN),
         owned(short_lin, 3, half).reshape(8, half * PS, CHAN)], axis=1)
    c_ff = min(nsp, raising.shape[1] // 128)
    F = raising.shape[1] // c_ff
    q_all, M = c_ff * q, ntp // 2
    cfg = (nsp, ntp, n, S, W, G, PL, PS, D, c_ff, F)
    vm = pl.BlockSpec(memory_space=pltpu.VMEM)
    dma = pltpu.SemaphoreType.DMA
    return pl.pallas_call(
        functools.partial(mixer_body, cfg),
        out_shape=jax.ShapeDtypeStruct((n, Dl), BF16),
        in_specs=[vm] * 9 + [pl.BlockSpec(memory_space=pl.ANY)] * 3,
        out_specs=vm,
        scratch_shapes=[
            pltpu.VMEM((n, S), F32), pltpu.VMEM((n, S), F32),
            pltpu.VMEM((n, 4 * S), F32), pltpu.VMEM((n, 4 * S), F32),
            pltpu.VMEM((8, SUB, S), F32), pltpu.VMEM((8, S), F32), pltpu.VMEM((nsp - 1, 8, S), F32),
            pltpu.VMEM((4, SUB, S), F32),
            pltpu.VMEM((ntp, q, W), BF16), pltpu.VMEM((ntp - 1, q, W), BF16),
            pltpu.VMEM((q, ntp * W), BF16), pltpu.VMEM(emitted.shape, BF16),
            pltpu.VMEM((ntp - 1, q, Dl), BF16),
            pltpu.VMEM((q, D), F32),
            pltpu.VMEM((ntp, nsp, D // nsp, F), BF16), pltpu.VMEM((ntp, nsp, F, D // nsp), BF16),
            pltpu.VMEM((c_ff, q, D), BF16), pltpu.VMEM((ntp, q_all, F), BF16),
            pltpu.VMEM((c_ff, q, D), BF16), pltpu.VMEM((c_ff - 1, q, D), BF16),
            pltpu.VMEM((ntp, q, Dl), BF16), pltpu.VMEM((ntp - 1, q, Dl), BF16),
            dma((3,)), dma((nsp - 1,)), dma((nsp - 1,)), dma((ntp - 1,)), dma((ntp - 1,)),
            dma((ntp - 1,)), dma((ntp - 1,)),
            *[dma((nsp - 1,))] * 4, *[dma((M - 1, nsp))] * 4, *[dma((M,))] * 4,
            *[dma((c_ff - 1,))] * 4, *[dma((ntp - 1,))] * 2,
        ],
        compiler_params=pltpu.CompilerParams(collective_id=0, has_side_effects=True),
        cost_estimate=pl.CostEstimate(flops=10**9, bytes_accessed=3 * 10**7, transcendentals=10**6),
    )(x, mix(dts), mix(fades), rates, lin, owned(skip, 0, W)[None], owned(closing, 0, W)[None],
      residual, leading[None], emitted, raising, lowering)


def solution(mesh):
    both, swapped = P("sp", "tp"), P("tp", "sp")
    in_specs = (both, both, swapped, swapped) + (P(),) * 10 + (both, swapped)
    return jax.shard_map(on_device, mesh=mesh, in_specs=in_specs, out_specs=both, check_vma=False)
```

```python
import functools

import jax
import jax.numpy as jnp
from jax import lax
from jax.experimental import pallas as pl
from jax.experimental.pallas import tpu as pltpu
from jax.sharding import PartitionSpec as P

CHAN = 16
NORM_W = 128
EPSILON = 1e-06
SUB = 8
F32, BF16 = jnp.float32, jnp.bfloat16


def sincos(a):
    k = jnp.floor(a * 0.6366197723675814 + 0.5)
    r = a - k * 1.5703125
    r = r - k * 4.8351287841796875e-4
    r = r - k * 3.138556210e-7
    z = r * r
    s = r + r * z * (-1.6666654611e-1 + z * (8.3321608736e-3 + z * -1.9515295891e-4))
    c = 1.0 - 0.5 * z + z * z * (
        4.166664568298827e-2 + z * (-1.388731625493765e-3 + z * 2.443315711809948e-5)
    )
    half = jnp.floor(k * 0.5)
    odd = (k - 2.0 * half) > 0.5
    half_odd = (half - 2.0 * jnp.floor(half * 0.5)) > 0.5
    cos_v = jnp.where(odd, -s, c)
    sin_v = jnp.where(odd, c, s)
    return jnp.where(half_odd, -cos_v, cos_v), jnp.where(half_odd, -sin_v, sin_v)


def one_minus_exp_neg(u):
    t = jnp.full_like(u, 1.0)
    for m in range(10, 1, -1):
        t = 1.0 - u * (1.0 / m) * t
    return u * t


def cmul(ar, ai, br, bi):
    return ar * br - ai * bi, ar * bi + ai * br


def mixer_body(cfg, x_ref, dt_ref, lf_ref, long_rate, short_rate, long_freq, short_freq,
               skip_ref, gain_ref, resid_ref, lead_ref, long_hbm, short_hbm, emit_hbm, up_hbm, down_hbm,
               out_ref, lin_l, lin_s, lin_sem,
               pace, surge, pre, st, blk, ends, ends_all, cin, mg, rows_in, mrg, emit, resid_in,
               mid_out, wup, wdn, nrm, hid, part, rs_in, fin, fin_in,
               copy_sem, s_ends, r_ends, s_rows, r_rows, s_res, r_res,
               s_u1, r_u1, s_d1, r_d1, s_u2, r_u2, s_d2, r_d2, s_u3, r_u3, s_d3, r_d3,
               s_nrm, r_nrm, s_rs, r_rs, s_fin, r_fin):
    nsp, ntp, n, S, W, G, PL, PS, D, c_ff, F = cfg
    M = ntp // 2
    L = n // SUB
    half = G // 2
    SL = half * PL
    sp = lax.axis_index("sp")
    tp = lax.axis_index("tp")
    q = n // ntp
    Dl = D // ntp
    MESH = pl.DeviceIdType.MESH

    emit_copy = pltpu.make_async_copy(emit_hbm, emit, copy_sem.at[0])
    lin_copies = []
    for at in range(8):
        for kind, (src, dst) in enumerate(((long_hbm, lin_l), (short_hbm, lin_s))):
            lin_copies.append(pltpu.make_async_copy(
                src.at[at // 4, at // 2 % 2, at % 2, pl.ds(tp * half, half)], dst.at[at],
                lin_sem.at[kind, at]))
    for copy in lin_copies:
        copy.start()
    emit_copy.start()
    chunk = lax.rem(sp, c_ff)
    partner = tp + 1 - 2 * lax.rem(tp, 2)

    def cols(of):
        return pl.ds(pl.multiple_of(of * F, 128), F)

    own_up = pltpu.make_async_copy(up_hbm.at[:, cols(chunk)], wup.at[tp, sp], copy_sem.at[1])
    own_down = pltpu.make_async_copy(down_hbm.at[cols(chunk), :], wdn.at[tp, sp], copy_sem.at[2])
    own_up.start()
    own_down.start()

    def spread_copy(k, up):
        to = lax.rem(sp + k, nsp)
        src = up_hbm.at[:, cols(lax.rem(to, c_ff))] if up else down_hbm.at[cols(lax.rem(to, c_ff)), :]
        return pltpu.make_async_remote_copy(
            src_ref=src, dst_ref=(wup if up else wdn).at[tp, sp],
            send_sem=(s_u1 if up else s_d1).at[k - 1], recv_sem=(r_u1 if up else r_d1).at[k - 1],
            device_id=(to, tp), device_id_type=MESH)

    def across_copy(m, k, up):
        piece = (wup if up else wdn).at[tp, lax.rem(sp - k + nsp, nsp)]
        return pltpu.make_async_remote_copy(
            src_ref=piece, dst_ref=piece,
            send_sem=(s_u2 if up else s_d2).at[m - 1, k], recv_sem=(r_u2 if up else r_d2).at[m - 1, k],
            device_id=(sp, lax.rem(tp + 2 * m, ntp)), device_id_type=MESH)

    def pair_copy(m, up):
        piece = (wup if up else wdn).at[lax.rem(tp + 2 * m, ntp)]
        return pltpu.make_async_remote_copy(
            src_ref=piece, dst_ref=piece,
            send_sem=(s_u3 if up else s_d3).at[m], recv_sem=(r_u3 if up else r_d3).at[m],
            device_id=(sp, partner), device_id_type=MESH)

    def pass_on(first, last, up):
        for k in range(first, last):
            if k == 0:
                (own_up if up else own_down).wait()
            else:
                spread_copy(k, up).wait_recv()
            for m in range(1, M):
                across_copy(m, k, up).start()

    barrier = pltpu.get_barrier_semaphore()
    for k in range(1, nsp):
        pl.semaphore_signal(barrier, inc=1, device_id=(lax.rem(sp + k, nsp), tp), device_id_type=MESH)
    for k in range(1, ntp):
        pl.semaphore_signal(barrier, inc=1, device_id=(sp, lax.rem(tp + k, ntp)), device_id_type=MESH)
    pl.semaphore_wait(barrier, nsp + ntp - 2)

    def res_copy(k):
        to = lax.rem(tp + k, ntp)
        return pltpu.make_async_remote_copy(
            src_ref=resid_ref.at[pl.ds(to * q, q), :], dst_ref=resid_in.at[k - 1],
            send_sem=s_res.at[k - 1], recv_sem=r_res.at[k - 1],
            device_id=(sp, to), device_id_type=MESH)

    for k in range(1, nsp):
        spread_copy(k, True).start()
    for k in range(1, ntp):
        res_copy(k).start()

    lane = lax.broadcasted_iota(jnp.int32, (G, S), 1)
    group = jnp.where(lane < SL, 2 * (lane // PL), 2 * ((lane - SL) // PS) + 1)
    spread = (group == lax.broadcasted_iota(jnp.int32, (G, S), 0)).astype(F32)
    r = lax.broadcasted_iota(jnp.int32, (n, n), 0)
    t = lax.broadcasted_iota(jnp.int32, (n, n), 1)
    mix = (t == (r % SUB) * L + r // SUB).astype(F32)

    def per_state(ref):
        moved = lax.dot_general(ref[...], mix, (((1,), (1,)), ((), ())),
                                precision=lax.Precision.HIGHEST, preferred_element_type=F32)
        return lax.dot_general(moved, spread, (((0,), (0,)), ((), ())),
                               precision=lax.Precision.HIGHEST, preferred_element_type=F32)

    pace[...] = per_state(dt_ref)
    surge[...] = per_state(lf_ref)

    def flat_kind(ref, e):
        many, states = ref.shape[1:]
        width = half * states
        repeat = (lax.broadcasted_iota(jnp.int32, (states, width), 1) % states
                  == lax.broadcasted_iota(jnp.int32, (states, width), 0)).astype(F32)
        wide = jnp.dot(ref[e], repeat, precision=lax.Precision.HIGHEST, preferred_element_type=F32)
        owner = tp * half + lax.broadcasted_iota(jnp.int32, (many, width), 1) // states
        mine = owner == lax.broadcasted_iota(jnp.int32, (many, width), 0)
        return jnp.sum(jnp.where(mine, wide, 0.0), axis=0, keepdims=True)

    def flat(long_ref, short_ref, e):
        return jnp.concatenate([flat_kind(long_ref, e), flat_kind(short_ref, e)], axis=1)

    def widened(ref, index, states, sign):
        rows, width = half * CHAN, half * states
        repeat = (lax.broadcasted_iota(jnp.int32, (states, width), 1) % states
                  == lax.broadcasted_iota(jnp.int32, (states, width), 0)).astype(BF16)
        wide = jnp.dot(ref[index].reshape(rows, states).astype(BF16), repeat, preferred_element_type=F32)
        own_block = (lax.broadcasted_iota(jnp.int32, (rows, width), 0) // CHAN
                     == lax.broadcasted_iota(jnp.int32, (rows, width), 1) // states)
        return jnp.where(own_block, sign * wide, 0.0).astype(BF16)

    def block_map(index, sign=1.0):
        long_part = widened(lin_l, index, PL, sign)
        short_part = widened(lin_s, index, PS, sign)
        no_long, no_short = jnp.zeros((CHAN, SL), BF16), jnp.zeros((CHAN, S - SL), BF16)
        bands = []
        for g in range(half):
            band = slice(g * CHAN, (g + 1) * CHAN)
            bands.append(jnp.concatenate([long_part[band], no_short], axis=1))
            bands.append(jnp.concatenate([no_long, short_part[band]], axis=1))
        return jnp.concatenate(bands, axis=0)

    xv = jnp.dot(mix.astype(BF16), x_ref[...], preferred_element_type=F32).astype(BF16)
    for copy in lin_copies:
        copy.wait()
    for e in range(2):
        for c in range(2):
            st[:, pl.ds((2 * e + c) * S, S)] = jnp.dot(
                xv, block_map(4 * e + c), preferred_element_type=F32)

    for e in range(2):
        rate = flat(long_rate, short_rate, e)
        freq = flat(long_freq, short_freq, e)

        def step(i, carry):
            pr, pi, sr, si = carry
            at = i if e == 0 else L - 1 - i
            rows = pl.ds(pl.multiple_of(at * SUB, SUB), SUB)
            d = pace[rows, :]
            rd = rate * d
            m = jnp.exp(surge[rows, :] - rd)
            cos_v, sin_v = sincos(freq * d)
            w = jnp.sqrt(one_minus_exp_neg(2.0 * rd))
            ar, ai = m * cos_v, m * sin_v
            pr, pi = cmul(ar, ai, pr, pi)
            sr, si = cmul(ar, ai, sr, si)
            sr = sr + w * st[rows, pl.ds(2 * e * S, S)]
            si = si + w * st[rows, pl.ds((2 * e + 1) * S, S)]
            pre[rows, pl.ds(2 * e * S, S)] = pr
            pre[rows, pl.ds((2 * e + 1) * S, S)] = pi
            st[rows, pl.ds(2 * e * S, S)] = sr
            st[rows, pl.ds((2 * e + 1) * S, S)] = si
            return pr, pi, sr, si

        zero = jnp.zeros((SUB, S), F32)
        total = lax.fori_loop(0, L, step, (zero + 1.0, zero, zero, zero))
        for c in range(4):
            blk[4 * e + c] = total[c]
        order = range(SUB) if e == 0 else range(SUB - 1, -1, -1)
        run = None
        for b in order:
            now = tuple(blk[4 * e + c, b : b + 1, :] for c in range(4))
            if run is None:
                run = now
            else:
                p = cmul(now[0], now[1], run[0], run[1])
                s = cmul(now[0], now[1], run[2], run[3])
                run = (p[0], p[1], s[0] + now[2], s[1] + now[3])
        for c in range(4):
            ends[4 * e + c : 4 * e + c + 1, :] = run[c]

    def ends_copy(k):
        return pltpu.make_async_remote_copy(
            src_ref=ends, dst_ref=ends_all.at[k - 1],
            send_sem=s_ends.at[k - 1], recv_sem=r_ends.at[k - 1],
            device_id=(lax.rem(sp + k, nsp), tp), device_id_type=MESH)

    for k in range(1, nsp):
        ends_copy(k).start()
    for k in range(1, nsp):
        spread_copy(k, False).start()

    read = jnp.concatenate(
        [block_map(2), block_map(3, -1.0), block_map(6), block_map(7, -1.0)], axis=1)

    pass_on(0, nsp // 2, True)
    for k in range(1, nsp):
        ends_copy(k).wait_recv()
    blank = jnp.zeros((1, S), F32)

    def fold(j, carry, e):
        cr, ci = carry
        k = nsp - 1 - j if e == 0 else j + 1
        reached = k <= sp if e == 0 else nsp - k <= nsp - 1 - sp
        got = ends_all[k - 1]
        nr, ni = cmul(got[4 * e : 4 * e + 1], got[4 * e + 1 : 4 * e + 2], cr, ci)
        nr = nr + got[4 * e + 2 : 4 * e + 3]
        ni = ni + got[4 * e + 3 : 4 * e + 4]
        return jnp.where(reached, nr, cr), jnp.where(reached, ni, ci)

    for e in range(2):
        cr, ci = lax.fori_loop(0, nsp - 1, functools.partial(fold, e=e), (blank, blank))
        order = range(SUB) if e == 0 else range(SUB - 1, -1, -1)
        for b in order:
            cin[2 * e, b : b + 1, :] = cr
            cin[2 * e + 1, b : b + 1, :] = ci
            now = tuple(blk[4 * e + c, b : b + 1, :] for c in range(4))
            nr, ni = cmul(now[0], now[1], cr, ci)
            cr, ci = nr + now[2], ni + now[3]

        inr, ini = cin[2 * e], cin[2 * e + 1]

        def settle(i, _):
            rows = pl.ds(pl.multiple_of(i * SUB, SUB), SUB)
            re, im = pl.ds(2 * e * S, S), pl.ds((2 * e + 1) * S, S)
            ar, ai = cmul(pre[rows, re], pre[rows, im], inr, ini)
            st[rows, re] = st[rows, re] + ar
            st[rows, im] = st[rows, im] + ai
            return 0

        lax.fori_loop(0, L, settle, 0)

    y = lax.dot_general(st[...].astype(BF16), read, (((1,), (1,)), ((), ())),
                        preferred_element_type=F32)
    own = pl.ds(pl.multiple_of(tp * W, 128), W)
    skip_row, gain_row = skip_ref[:, own], gain_ref[:, own]
    y = y + skip_row * xv.astype(F32)
    y = 0.5 * y * (1.0 + jnp.tanh(0.7978845608028654 * (y + 0.044715 * y * y * y)))
    heads = []
    for h in range(W // NORM_W):
        head = y[:, h * NORM_W : (h + 1) * NORM_W]
        scale = lax.rsqrt(jnp.mean(head * head, axis=1, keepdims=True) + EPSILON)
        heads.append(head * scale * gain_row[:, h * NORM_W : (h + 1) * NORM_W])
    merged = jnp.concatenate(heads, axis=1).astype(BF16)
    t = lax.broadcasted_iota(jnp.int32, (n, n), 0)
    r = lax.broadcasted_iota(jnp.int32, (n, n), 1)
    unmix = (r == (t % L) * SUB + t // L).astype(BF16)
    mg[...] = jnp.dot(unmix, merged, preferred_element_type=F32).astype(BF16).reshape(ntp, q, W)

    def row_copy(k):
        to = lax.rem(tp + k, ntp)
        return pltpu.make_async_remote_copy(
            src_ref=mg.at[to], dst_ref=rows_in.at[k - 1],
            send_sem=s_rows.at[k - 1], recv_sem=r_rows.at[k - 1],
            device_id=(sp, to), device_id_type=MESH)

    for k in range(1, ntp):
        row_copy(k).start()
    pass_on(nsp // 2, nsp, True)
    emit_copy.wait()
    mrg[:, pl.ds(pl.multiple_of(tp * W, 128), W)] = mg[tp]
    mid_out[:, pl.ds(pl.multiple_of(tp * Dl, 128), Dl)] = resid_ref[pl.ds(pl.multiple_of(tp * q, q), q), :].astype(F32)
    for k in range(1, ntp):
        src = lax.rem(tp - k + ntp, ntp)
        res_copy(k).wait_recv()
        mid_out[:, pl.ds(pl.multiple_of(src * Dl, 128), Dl)] = resid_in[k - 1].astype(F32)
        row_copy(k).wait_recv()
        mrg[:, pl.ds(pl.multiple_of(src * W, 128), W)] = rows_in[k - 1]
    mid = mid_out[...] + jnp.dot(mrg[...], emit[...], preferred_element_type=F32)
    mid_out[...] = mid
    scale = lax.rsqrt(jnp.mean(mid * mid, axis=1, keepdims=True) + EPSILON)
    base, q_all = sp - chunk, c_ff * q
    nrm[chunk] = (mid * scale * lead_ref[...]).astype(BF16)

    def peer(k):
        return lax.rem(chunk + k, c_ff)

    H = c_ff // 2

    def nrm_across(m):
        return pltpu.make_async_remote_copy(
            src_ref=nrm.at[chunk], dst_ref=nrm.at[chunk],
            send_sem=s_nrm.at[0, m], recv_sem=r_nrm.at[0, m],
            device_id=(base + peer(2 * m), tp), device_id_type=MESH)

    def nrm_pair(m):
        return pltpu.make_async_remote_copy(
            src_ref=nrm.at[peer(2 * m)], dst_ref=nrm.at[peer(2 * m)],
            send_sem=s_nrm.at[1, m], recv_sem=r_nrm.at[1, m],
            device_id=(base + chunk + 1 - 2 * lax.rem(chunk, 2), tp), device_id_type=MESH)

    def rs_copy(k):
        return pltpu.make_async_remote_copy(
            src_ref=part.at[peer(k)], dst_ref=rs_in.at[k - 1],
            send_sem=s_rs.at[k - 1], recv_sem=r_rs.at[k - 1],
            device_id=(base + peer(k), tp), device_id_type=MESH)

    def fin_copy(k):
        to = lax.rem(tp + k, ntp)
        return pltpu.make_async_remote_copy(
            src_ref=fin.at[to], dst_ref=fin_in.at[k - 1],
            send_sem=s_fin.at[k - 1], recv_sem=r_fin.at[k - 1],
            device_id=(sp, to), device_id_type=MESH)

    for m in range(1, H):
        nrm_across(m).start()
    nrm_pair(0).start()
    pair_copy(0, True).start()
    pass_on(0, nsp, False)
    pair_copy(0, False).start()
    for m in range(1, H):
        nrm_across(m).wait_recv()
        nrm_pair(H - m).start()
    for up in (True, False):
        for m in range(1, M):
            for k in range(nsp):
                across_copy(m, k, up).wait_recv()
            pair_copy(M - m, up).start()
        if up:
            for m in range(M):
                pair_copy(m, True).wait_recv()
            for m in range(H):
                nrm_pair(m).wait_recv()
            rows = nrm[...].reshape(q_all, D)

            def raise_step(t, _):
                upward = jnp.dot(rows, wup[t].reshape(D, F), preferred_element_type=F32)
                hid[t] = jnp.square(jnp.maximum(upward, 0.0)).astype(BF16)
                return 0

            lax.fori_loop(0, ntp, raise_step, 0)
    for m in range(M):
        pair_copy(m, False).wait_recv()
    Dc = D // nsp
    for j in range(nsp):
        total = jnp.dot(hid[0], wdn[0, j], preferred_element_type=F32)
        for t in range(1, ntp):
            total = total + jnp.dot(hid[t], wdn[t, j], preferred_element_type=F32)
        part[:, :, j * Dc : (j + 1) * Dc] = total.astype(BF16).reshape(c_ff, q, Dc)
    for k in range(1, c_ff):
        rs_copy(k).start()
    result = mid_out[...] + part[chunk].astype(F32)
    for k in range(1, c_ff):
        rs_copy(k).wait_recv()
        result = result + rs_in[k - 1].astype(F32)
    result = result.astype(BF16)
    for t in range(ntp):
        fin[t] = result[:, t * Dl : (t + 1) * Dl]
    for k in range(1, ntp):
        fin_copy(k).start()
    out_ref[pl.ds(pl.multiple_of(tp * q, q), q), :] = fin[tp]
    for k in range(1, ntp):
        fin_copy(k).wait_recv()
        src = lax.rem(tp - k + ntp, ntp)
        out_ref[pl.ds(pl.multiple_of(src * q, q), q), :] = fin_in[k - 1]
    for k in range(1, c_ff):
        rs_copy(k).wait_send()
    for m in range(H):
        if m > 0:
            nrm_across(m).wait_send()
        nrm_pair(m).wait_send()
    for k in range(1, ntp):
        fin_copy(k).wait_send()
    for up in (True, False):
        for k in range(1, nsp):
            spread_copy(k, up).wait_send()
        for m in range(1, M):
            for k in range(nsp):
                across_copy(m, k, up).wait_send()
        for m in range(M):
            pair_copy(m, up).wait_send()
    for k in range(1, nsp):
        ends_copy(k).wait_send()
    for k in range(1, ntp):
        res_copy(k).wait_send()
        row_copy(k).wait_send()


def on_device(residual, lifted, dts, fades, long_rate, short_rate, long_freq, short_freq,
              long_lin, short_lin, skip, closing, emitted, leading, raising, lowering):
    nsp, ntp = lax.axis_size("sp"), lax.axis_size("tp")
    n, W = lifted.shape
    G = dts.shape[0]
    half = G // 2
    PL, PS = long_rate.shape[2], short_rate.shape[2]
    S = half * (PL + PS)
    D = emitted.shape[1]
    Dl = residual.shape[1]
    q = n // ntp
    c_ff = min(nsp, raising.shape[1] // 128)
    F = raising.shape[1] // c_ff
    q_all, M = c_ff * q, ntp // 2
    cfg = (nsp, ntp, n, S, W, G, PL, PS, D, c_ff, F)
    vm = pl.BlockSpec(memory_space=pltpu.VMEM)
    dma = pltpu.SemaphoreType.DMA
    return pl.pallas_call(
        functools.partial(mixer_body, cfg),
        out_shape=jax.ShapeDtypeStruct((n, Dl), BF16),
        in_specs=[vm] * 11 + [pl.BlockSpec(memory_space=pl.ANY)] * 5,
        out_specs=vm,
        scratch_shapes=[
            pltpu.VMEM((8, half, CHAN, PL), F32), pltpu.VMEM((8, half, CHAN, PS), F32), dma((2, 8)),
            pltpu.VMEM((n, S), F32), pltpu.VMEM((n, S), F32),
            pltpu.VMEM((n, 4 * S), F32), pltpu.VMEM((n, 4 * S), F32),
            pltpu.VMEM((8, SUB, S), F32), pltpu.VMEM((8, S), F32), pltpu.VMEM((nsp - 1, 8, S), F32),
            pltpu.VMEM((4, SUB, S), F32),
            pltpu.VMEM((ntp, q, W), BF16), pltpu.VMEM((ntp - 1, q, W), BF16),
            pltpu.VMEM((q, ntp * W), BF16), pltpu.VMEM(emitted.shape, BF16),
            pltpu.VMEM((ntp - 1, q, Dl), BF16),
            pltpu.VMEM((q, D), F32),
            pltpu.VMEM((ntp, nsp, D // nsp, F), BF16), pltpu.VMEM((ntp, nsp, F, D // nsp), BF16),
            pltpu.VMEM((c_ff, q, D), BF16), pltpu.VMEM((ntp, q_all, F), BF16),
            pltpu.VMEM((c_ff, q, D), BF16), pltpu.VMEM((c_ff - 1, q, D), BF16),
            pltpu.VMEM((ntp, q, Dl), BF16), pltpu.VMEM((ntp - 1, q, Dl), BF16),
            dma((3,)), dma((nsp - 1,)), dma((nsp - 1,)), dma((ntp - 1,)), dma((ntp - 1,)),
            dma((ntp - 1,)), dma((ntp - 1,)),
            *[dma((nsp - 1,))] * 4, *[dma((M - 1, nsp))] * 4, *[dma((M,))] * 4,
            *[dma((2, c_ff // 2))] * 2, *[dma((c_ff - 1,))] * 2, *[dma((ntp - 1,))] * 2,
        ],
        compiler_params=pltpu.CompilerParams(collective_id=0, has_side_effects=True),
        cost_estimate=pl.CostEstimate(flops=10**9, bytes_accessed=3 * 10**7, transcendentals=10**6),
    )(lifted, dts, fades, long_rate, short_rate, long_freq, short_freq, skip[None], closing[None],
      residual, leading[None], long_lin.swapaxes(4, 5), short_lin.swapaxes(4, 5), emitted, raising, lowering)


def solution(mesh):
    both, swapped = P("sp", "tp"), P("tp", "sp")
    in_specs = (both, both, swapped, swapped) + (P(),) * 10 + (both, swapped)
    return jax.shard_map(on_device, mesh=mesh, in_specs=in_specs, out_specs=both, check_vma=False)
```
